32 devices in a mesh: ep: 4 (over y, x), tp: 8 (over z, core).
Axes of the slice: x: 2, y: 2, z: 4, core: 2. Of those that a mesh axis runs over, the one named last changes fastest.
Arguments:
- queries: bfloat16 [2048, 1024], P('ep', 'tp'), may hold values from -30 to 30
- key_vectors: bfloat16 [2048, 1024], P('ep', 'tp'), may hold values from -30 to 30
- value_vectors: bfloat16 [2048, 1024], P('ep', 'tp'), may hold values from -9 to 9
- cumulative_gate: float32 [2048, 16], P('ep', 'tp'), as said below
- out_weight: bfloat16 [1024, 2048], P('tp'), may hold values from -0.1875 to 0.1875
- expert_tokens: bfloat16 [3072, 2048], P(('ep', 'tp')), may hold values from -6 to 6
- norm_gain: float32 [2048], replicated, may hold values from 0.1 to 1.9
- gate_weight: bfloat16 [16, 2048, 2048], P('ep', None, 'tp'), may hold values from -0.375 to 0.375
- up_weight: bfloat16 [16, 2048, 2048], P('ep', None, 'tp'), may hold values from -0.375 to 0.375
- down_weight: bfloat16 [16, 2048, 2048], P('ep', 'tp'), may hold values from -0.015625 to 0.015625
- expert_choice: int32 [3072, 2], P(('ep', 'tp')), may hold values from 0 to 15, all different within a row; in each aligned block of 96 rows (0 to 95, 96 to 191, ...) at most 13 rows name the same one
- route_weights: float32 [3072, 2], P(('ep', 'tp')), may hold values from 0.2 to 1
Outputs:
- mixer_output: bfloat16 [2048, 2048], P(('ep', 'tp'))
- expert_output: bfloat16 [3072, 2048], P(('ep', 'tp'))
The draws below stay inside these ranges and needn't reach their ends.
Inputs may be any that keep to these rules, and one draw needn't show every extreme that they name: `cumulative_gate`: each head's values never rise from one position to the next. `expert_choice`: each row names 2 different experts; within the rows of one device no expert is named more than 13 times, and in some of them one expert exactly 13 times.
All inputs are finite; a program needn't handle non-finite values.
Results may differ from the reference program's by a relative error of at most 0.019.
Values may be sent and summed in bfloat16 or wider, within the bound.
A program may use at most 128 MiB of HBM per device.

```python
import math
import jax
import jax.numpy as jnp
import numpy as np
from jax import lax

D = 2048
HEAD_DIM = 64
HEAD_COUNT = 16
FF = 2048
EXPERTS = 16
TOPK = 2
TOK_DEV = 96
CAP = 13
ROWS = 512
TOKEN_POSITIONS = 2048
EXP_TOKENS = 3072
N_TP = 8


def paired_vectors(key):
    full_width = HEAD_COUNT * HEAD_DIM
    query_key = jax.random.fold_in(key, 101)
    vector_key = jax.random.fold_in(key, 102)
    queries = jnp.clip(jax.random.normal(query_key, (TOKEN_POSITIONS, full_width), jnp.float32), -6.0, 6.0)
    vectors = jnp.clip(jax.random.normal(vector_key, (TOKEN_POSITIONS, full_width), jnp.float32), -6.0, 6.0)
    return (queries, vectors)


def draw_queries(key, part):
    return paired_vectors(key)[0].astype(jnp.bfloat16)


def draw_key_vectors(key, part):
    return paired_vectors(key)[1].astype(jnp.bfloat16)


def draw_cumulative_gate(key, part):
    fast_share = 0.5
    head_draw = jax.random.uniform(jax.random.fold_in(key, 201), (HEAD_COUNT,), jnp.float32)
    fast_rate = jnp.exp(jax.random.uniform(jax.random.fold_in(key, 202), (HEAD_COUNT,), jnp.float32, math.log(0.012), math.log(0.035)))
    slow_rate = jnp.exp(jax.random.uniform(jax.random.fold_in(key, 203), (HEAD_COUNT,), jnp.float32, math.log(0.1), math.log(0.5))) / TOKEN_POSITIONS
    head_rate = jnp.where(head_draw < fast_share, fast_rate, slow_rate)
    block_count = TOKEN_POSITIONS // ROWS
    block_factor = jnp.exp(jax.random.uniform(jax.random.fold_in(key, 204), (block_count,), jnp.float32, math.log(0.4), math.log(2.5)))
    position_factor = jnp.repeat(block_factor, ROWS)
    roughness = jax.random.uniform(jax.random.fold_in(key, 205), (TOKEN_POSITIONS, HEAD_COUNT), jnp.float32, 0.3, 1.7)
    logarithm_gate = -head_rate[None, :] * position_factor[:, None] * roughness
    spike_rows = jax.random.randint(jax.random.fold_in(key, 206), (3,), 0, TOKEN_POSITIONS)
    spike_loss = jax.random.uniform(jax.random.fold_in(key, 207), (3, HEAD_COUNT), jnp.float32, 0.2, 0.4)
    logarithm_gate = logarithm_gate.at[spike_rows].add(jnp.log1p(-spike_loss))
    return jnp.cumsum(logarithm_gate, axis=0)


def block_levels(key, dims, cuts, smallest, high):
    loudness = 1.0
    for position, shards_of in cuts:
        draws = jax.random.uniform(jax.random.fold_in(jax.random.fold_in(key, 6), position), (shards_of,), jnp.float32, smallest / len(cuts), high / len(cuts))
        loudness = loudness * jnp.repeat(jnp.exp(draws), dims[position] // shards_of).reshape((-1,) + (1,) * (len(dims) - 1 - position))
    return loudness


def deal_out(stream_key, own, number, rows, amount, top, limit, lean):
    order = jax.random.permutation(stream_key, amount)
    crowded, usual = shares(amount, rows * top, limit, lean, True), shares(amount, rows * top, limit, lean, False)
    places = jnp.arange(amount)

    def named(tallies, rotation):
        used = int((tallies > 0).sum())
        fixed = max(1, used // 4)
        moved = fixed + (places - fixed + rotation * (used - fixed)) % max(1, amount - fixed)
        return jnp.zeros((amount,), jnp.int32).at[order[jnp.where(places < fixed, places, moved)]].set(jnp.asarray(tallies, jnp.int32))

    tallies = jnp.where(number % 4 == 0, named(crowded, number // 4), named(usual, number - number // 4 - 1))
    mixed = jax.random.permutation(jax.random.fold_in(own, 3), amount)
    giver, sink = mixed[0:amount // 2 * 2:2], mixed[1:amount // 2 * 2:2]
    room = jnp.minimum(tallies[giver] - 1, limit - tallies[sink]) // 2
    room = jnp.where((giver == order[0]) | (sink == order[0]) | (tallies[sink] == 0), 0, jnp.maximum(room, 0))
    moved = jax.random.randint(jax.random.fold_in(own, 4), (amount // 2,), 0, 1 << 20) % (room + 1)
    tallies = tallies.at[giver].add(-moved).at[sink].add(moved)
    items = jnp.searchsorted(jnp.cumsum(tallies), jnp.arange(rows * top), side="right").astype(jnp.int32)
    table = items.reshape(top, rows).T
    table = table[jax.random.permutation(jax.random.fold_in(own, 1), rows)]
    rotation = jax.random.randint(jax.random.fold_in(own, 2), (rows, 1), 0, top)
    return jnp.take_along_axis(table, (jnp.arange(top)[None, :] + rotation) % top, axis=1)


def shares(amount, total, bound, skew, full):
    weights = [(1 << 20) // math.isqrt(grade ** skew) + 1 for grade in range(1, amount + 1)]
    largest = bound if full else min(bound, max(-(-total // amount), total * weights[0] // sum(weights)))
    least = 1 if total - largest >= amount - 1 else 0
    counts, surplus = [largest] + [least] * (amount - 1), total - largest - least * (amount - 1)
    while surplus > 0:
        free = [i for i in range(1, amount) if counts[i] < largest] or [i for i in range(1, amount) if counts[i] < bound]
        mass, remaining = sum([weights[i] for i in free]), surplus
        for i in free:
            more = min(bound - counts[i], max(1, remaining * weights[i] // mass), surplus)
            counts[i] = counts[i] + more
            surplus = surplus - more
    return np.array(counts)


def scatter_about(own_key, dims, scale, bound, shards=(), held_as=jnp.bfloat16):
    array = jax.random.normal(own_key, dims, jnp.float32) * scale
    if len(shards) > 0:
        array = block_levels(own_key, dims, shards, -0.22, 0.18) * array
    return jnp.clip(array, min=-bound, max=bound).astype(held_as)


def setup_inputs(seed: int = 0) -> dict:
    keys = jax.random.split(jax.random.key(seed), 13)
    queries = draw_queries(jax.random.fold_in(keys[12], 71), 0)
    key_vectors = draw_key_vectors(jax.random.fold_in(keys[12], 71), 0)
    value_vectors = scatter_about(keys[2], (TOKEN_POSITIONS, HEAD_COUNT * HEAD_DIM), 1.5, 9.0, ((0, 4), (1, 8)))
    cumulative_gate = draw_cumulative_gate(jax.random.fold_in(keys[12], 71), 0)
    out_weight = scatter_about(keys[4], (HEAD_COUNT * HEAD_DIM, D), (HEAD_COUNT * HEAD_DIM) ** -0.5, 0.1875, ((0, 8),))
    expert_tokens = scatter_about(keys[5], (EXP_TOKENS, D), 1.0, 6.0, ((0, 32),))
    norm_gain = jnp.clip(1.0 + 0.18 * jax.random.normal(keys[6], (D,), jnp.float32), 0.1, 1.9)
    gate_weight = scatter_about(keys[7], (EXPERTS, D, FF), (D // 9) ** -0.5, 0.375, ((0, 4), (2, 8)))
    up_weight = scatter_about(keys[8], (EXPERTS, D, FF), (D // 9) ** -0.5, 0.375, ((0, 4), (2, 8)))
    down_weight = scatter_about(keys[9], (EXPERTS, FF, D), (FF * 64) ** -0.5, 0.015625, ((0, 4), (1, 8)))
    expert_choice_keys = jax.random.split(jax.random.fold_in(keys[10], 1), EXP_TOKENS // TOK_DEV)
    expert_choice_turns = jax.random.permutation(jax.random.fold_in(keys[10], 3), EXP_TOKENS // TOK_DEV)
    expert_choice = jax.vmap(lambda own, number: deal_out(jax.random.fold_in(keys[10], 2), own, number, TOK_DEV, EXPERTS, TOPK, CAP, 1))(expert_choice_keys, expert_choice_turns).reshape((EXP_TOKENS, TOPK))
    route_weights = jnp.clip(0.2 + 0.8 * jax.random.uniform(keys[11], (EXP_TOKENS, TOPK), jnp.float32) ** block_levels(keys[11], (EXP_TOKENS, TOPK), ((0, 32),), -0.2, 0.2), 0.2, 1.0)
    return {"queries": queries, "key_vectors": key_vectors, "value_vectors": value_vectors, "cumulative_gate": cumulative_gate, "out_weight": out_weight, "expert_tokens": expert_tokens, "norm_gain": norm_gain, "gate_weight": gate_weight, "up_weight": up_weight, "down_weight": down_weight, "expert_choice": expert_choice, "route_weights": route_weights}


eps_norm = 1e-05
clamp_limit = 7.0
sig_alpha = 1.702

def mixer_part(queries, key_vectors, value_vectors, cumulative_gate, out_weight):
    total_rows = queries.shape[0]
    block_size = min(512, total_rows)
    block_count = total_rows // block_size
    score_scale = 1.0 / math.sqrt(HEAD_DIM)
    key_pos = jnp.arange(total_rows, dtype=jnp.int32)

    def single_head(head_index):
        first_column = (head_index * HEAD_DIM).astype(jnp.int32)
        head_queries = lax.dynamic_slice_in_dim(queries, first_column, HEAD_DIM, 1)
        head_keys = lax.dynamic_slice_in_dim(key_vectors, first_column, HEAD_DIM, 1)
        head_values = lax.dynamic_slice_in_dim(value_vectors, first_column, HEAD_DIM, 1)
        head_gates = lax.dynamic_slice_in_dim(cumulative_gate, head_index.astype(jnp.int32), 1, 1)[:, 0]

        def one_block(block_index):
            row_start = (block_index * block_size).astype(jnp.int32)
            block_queries = lax.dynamic_slice_in_dim(head_queries, row_start, block_size, 0)
            block_gates = lax.dynamic_slice_in_dim(head_gates, row_start, block_size, 0)
            scores = jnp.dot(block_queries, head_keys.T, preferred_element_type=jnp.float32) * score_scale
            scores = scores + block_gates[:, None] - head_gates[None, :]
            query_pos = row_start + jnp.arange(block_size, dtype=jnp.int32)
            causal = key_pos[None, :] <= query_pos[:, None]
            scores = jnp.where(causal, scores, -jnp.inf)
            row_peak = lax.optimization_barrier(jnp.max(scores, axis=1, keepdims=True))
            weights = jnp.where(causal, jnp.exp(scores - row_peak), 0.0)
            numer = jnp.dot(weights.astype(jnp.bfloat16), head_values, preferred_element_type=jnp.float32)
            return (numer / lax.optimization_barrier(jnp.sum(weights, axis=1, keepdims=True))).astype(jnp.bfloat16)
        return lax.map(one_block, jnp.arange(block_count, dtype=jnp.int32)).reshape(total_rows, HEAD_DIM)
    per_head = lax.map(single_head, jnp.arange(HEAD_COUNT, dtype=jnp.int32))
    attention = jnp.transpose(per_head, (1, 0, 2)).reshape(total_rows, HEAD_COUNT * HEAD_DIM)
    group_width = HEAD_COUNT // N_TP * HEAD_DIM

    def add_group(running_total, group_index):
        first_column = (group_index * group_width).astype(jnp.int32)
        columns = lax.dynamic_slice_in_dim(attention, first_column, group_width, 1)
        weight_rows = lax.dynamic_slice_in_dim(out_weight, first_column, group_width, 0)
        partial_sum = jnp.dot(columns, weight_rows, preferred_element_type=jnp.float32).astype(jnp.bfloat16)
        partial_sum = lax.optimization_barrier(partial_sum)
        return (running_total + partial_sum.astype(jnp.float32), None)
    summed, unused = lax.scan(add_group, jnp.zeros((total_rows, D), jnp.float32), jnp.arange(N_TP, dtype=jnp.int32))
    return summed.astype(jnp.bfloat16)

def expert_part(expert_tokens, norm_gain, gate_weight, up_weight, down_weight, expert_choice, route_weights):
    total_rows = expert_tokens.shape[0]
    block_count = total_rows // TOK_DEV
    tokens_float = expert_tokens.astype(jnp.float32)
    normed = (tokens_float * lax.rsqrt(lax.optimization_barrier(jnp.mean(tokens_float * tokens_float, axis=1, keepdims=True)) + eps_norm) * norm_gain).astype(jnp.bfloat16)
    flat_ids = expert_choice.reshape(block_count, TOK_DEV * TOPK).astype(jnp.int32)
    one_hot = (flat_ids[:, :, None] == jnp.arange(EXPERTS, dtype=jnp.int32)[None, None, :]).astype(jnp.int32)
    slot_rank = lax.optimization_barrier(jnp.sum((jnp.cumsum(one_hot, axis=1) - one_hot) * one_hot, axis=2))
    block_ids = jnp.arange(block_count, dtype=jnp.int32)[:, None]
    destination = (flat_ids * (block_count * CAP) + block_ids * CAP + slot_rank).reshape(-1)
    token_ids = (block_ids * TOK_DEV + jnp.arange(TOK_DEV * TOPK, dtype=jnp.int32)[None, :] // TOPK).reshape(-1)
    slot_rows = jnp.zeros((EXPERTS * block_count * CAP, D), jnp.bfloat16).at[destination].set(normed[token_ids])
    slot_rows = slot_rows.reshape(EXPERTS, block_count * CAP, D)
    unit_group = FF // N_TP

    def single_expert(operands):
        rows_in, gate_matrix, up_matrix, down_matrix = operands
        gate_pre = jnp.minimum(jnp.dot(rows_in, gate_matrix, preferred_element_type=jnp.float32), clamp_limit)
        up_pre = jnp.clip(jnp.dot(rows_in, up_matrix, preferred_element_type=jnp.float32), -clamp_limit, clamp_limit)
        activation = (gate_pre * jax.nn.sigmoid(sig_alpha * gate_pre) * (up_pre + 1.0)).astype(jnp.bfloat16)

        def add_group(running_total, group_index):
            first_unit = (group_index * unit_group).astype(jnp.int32)
            columns = lax.dynamic_slice_in_dim(activation, first_unit, unit_group, 1)
            weight_rows = lax.dynamic_slice_in_dim(down_matrix, first_unit, unit_group, 0)
            partial_sum = jnp.dot(columns, weight_rows, preferred_element_type=jnp.float32).astype(jnp.bfloat16)
            partial_sum = lax.optimization_barrier(partial_sum)
            return (running_total + partial_sum.astype(jnp.float32), None)
        summed, unused = lax.scan(add_group, jnp.zeros((rows_in.shape[0], D), jnp.float32), jnp.arange(N_TP, dtype=jnp.int32))
        return summed.astype(jnp.bfloat16)
    results = lax.map(single_expert, (slot_rows, gate_weight, up_weight, down_weight)).reshape(EXPERTS * block_count * CAP, D)
    picked = results[destination].astype(jnp.float32).reshape(total_rows, TOPK, D)
    return lax.optimization_barrier(jnp.sum(picked * route_weights[:, :, None], axis=1)).astype(jnp.bfloat16)

def reference(queries, key_vectors, value_vectors, cumulative_gate, out_weight, expert_tokens, norm_gain, gate_weight, up_weight, down_weight, expert_choice, route_weights):
    mixer_output = mixer_part(queries, key_vectors, value_vectors, cumulative_gate, out_weight)
    expert_output = expert_part(expert_tokens, norm_gain, gate_weight, up_weight, down_weight, expert_choice, route_weights)
    return (mixer_output, expert_output)
```

```python
import functools
import math

import jax
import jax.numpy as jnp
from jax import lax
from jax.experimental import pallas as pl
from jax.experimental.pallas import tpu as pltpu
from jax.sharding import PartitionSpec as P

SLOTS = 16
CORES = 2
MESH = pl.DeviceIdType.MESH


eps_norm = 1e-05
clamp_limit = 7.0
sig_alpha = 1.702
floor_score = -1e30


def attend_shard(
    carried, queries, query_gates, query_pos, key_rows, value_rows, key_gates, key_start
):
    running_max, running_sum, accum = carried
    heads_here = query_gates.shape[1]
    head_width = queries.shape[1] // heads_here
    score_scale = 1.0 / math.sqrt(head_width)
    key_pos = key_start + jnp.arange(key_rows.shape[0], dtype=jnp.int32)
    causal = key_pos[None, :] <= query_pos[:, None]
    maxima = []
    totals = []
    blocks = []
    for head_index in range(heads_here):
        first_column = head_index * head_width
        last_column = first_column + head_width
        scores = (
            jnp.einsum(
                "qd,kd->qk",
                queries[:, first_column:last_column],
                key_rows[:, first_column:last_column],
                preferred_element_type=jnp.float32,
            )
            * score_scale
        )
        scores = (
            scores + query_gates[:, head_index : head_index + 1] - key_gates[:, head_index][None, :]
        )
        scores = jnp.where(causal, scores, floor_score)
        new_peak = jnp.maximum(running_max[head_index], jnp.max(scores, axis=1))
        weights = jnp.where(causal, jnp.exp(scores - new_peak[:, None]), 0.0)
        shrink = jnp.exp(running_max[head_index] - new_peak)
        maxima.append(new_peak)
        totals.append(running_sum[head_index] * shrink + jnp.sum(weights, axis=1))
        blocks.append(
            accum[:, first_column:last_column] * shrink[:, None]
            + jnp.dot(
                weights.astype(jnp.bfloat16),
                value_rows[:, first_column:last_column],
                preferred_element_type=jnp.float32,
            )
        )
    return (jnp.stack(maxima), jnp.stack(totals), jnp.concatenate(blocks, axis=1))


def head_term(attention, out_weight):
    return jnp.dot(attention, out_weight, preferred_element_type=jnp.float32)


def greet(e, t, ep, nz):
    z, c = t // CORES, t % CORES
    barrier = pltpu.get_barrier_semaphore()
    peers = [(e, z * CORES + 1 - c)]
    peers += [(e, lax.rem(z + k, nz) * CORES + c) for k in range(1, nz)]
    peers += [(lax.rem(e + j, ep), t) for j in range(1, ep)]
    for peer in peers:
        pl.semaphore_signal(barrier, inc=1, device_id=peer, device_id_type=MESH)
    pl.semaphore_wait(barrier, len(peers))


def dispatch_kernel(
    ep, nz, local_experts, x_ref, meta_ref, out_ref, metas_ref, xbuf, outbox,
    xs, xr, ms, mr, cs, cr, ds, dr,
):
    e, t = lax.axis_index("ep"), lax.axis_index("tp")
    z, c = t // CORES, t % CORES
    partner = (e, z * CORES + 1 - c)
    rows = x_ref.shape[0]
    greet(e, t, ep, nz)

    def token_copy(k):
        dest = (e, lax.rem(z + k, nz) * CORES + c)
        return (
            pltpu.make_async_remote_copy(
                src_ref=meta_ref, dst_ref=metas_ref.at[k], send_sem=ms.at[k], recv_sem=mr.at[k],
                device_id=dest, device_id_type=MESH,
            ),
            pltpu.make_async_remote_copy(
                src_ref=x_ref, dst_ref=xbuf.at[k], send_sem=xs.at[k], recv_sem=xr.at[k],
                device_id=dest, device_id_type=MESH,
            ),
        )

    def origin(k):
        return lax.rem(z - k + nz, nz)

    def row_copy(k, j):
        return pltpu.make_async_remote_copy(
            src_ref=outbox.at[k, lax.rem(e + j, ep)], dst_ref=out_ref.at[:, c, e, origin(k)],
            send_sem=cs.at[k, j], recv_sem=cr.at[k, j],
            device_id=(lax.rem(e + j, ep), t), device_id_type=MESH,
        )

    def share_copy(k, j):
        source = out_ref.at[:, c, lax.rem(e - j + ep, ep), origin(k)]
        return pltpu.make_async_remote_copy(
            src_ref=source, dst_ref=source, send_sem=ds.at[k, j], recv_sem=dr.at[k, j],
            device_id=partner, device_id_type=MESH,
        )

    order = sorted(range(1, nz), key=lambda k: min(k, nz - k))
    for k in order:
        for copy in token_copy(k):
            copy.start()
    far_first = [2] + [j for j in range(1, ep) if j != 2] if ep > 2 else list(range(1, ep))
    metas_ref[0] = meta_ref[...]
    for n, k in enumerate([0] + order):
        if k > 0:
            for copy in token_copy(k):
                copy.wait_recv()
        block = x_ref if k == 0 else xbuf.at[k]
        info = metas_ref[k]
        slot = lax.broadcasted_iota(jnp.int32, (ep * local_experts * SLOTS, rows), 0).astype(
            jnp.float32
        )
        chosen = (slot == info[0:1, :rows]) | (slot == info[1:2, :rows])
        picked = jnp.dot(
            jnp.where(chosen, 1.0, 0.0).astype(jnp.bfloat16), block[...],
            preferred_element_type=jnp.float32,
        ).astype(jnp.bfloat16)
        outbox[k] = picked.reshape(ep, local_experts, SLOTS, picked.shape[1])
        for j in far_first:
            row_copy(k, j).start()
        out_ref[:, c, e, origin(k)] = outbox[k, e]
        share_copy(k, 0).start()
    for k in [0] + order:
        for j in range(1, ep):
            row_copy(k, j).wait_recv()
            share_copy(k, j).start()
    for k in range(nz):
        for j in range(ep):
            share_copy(k, j).wait_send()
            other = out_ref.at[:, 1 - c, lax.rem(e - j + ep, ep), origin(k)]
            pltpu.make_async_remote_copy(
                src_ref=other, dst_ref=other, send_sem=ds.at[k, j], recv_sem=dr.at[k, j],
                device_id=partner, device_id_type=MESH,
            ).wait_recv()
            if j > 0:
                row_copy(k, j).wait_send()
        if k > 0:
            for copy in token_copy(k):
                copy.wait_send()


def dispatch(x, meta, ep, nz, local_experts):
    width = x.shape[1]
    dma = pltpu.SemaphoreType.DMA
    return pl.pallas_call(
        functools.partial(dispatch_kernel, ep, nz, local_experts),
        out_shape=(
            jax.ShapeDtypeStruct((local_experts, CORES, ep, nz, SLOTS, width), jnp.bfloat16),
            jax.ShapeDtypeStruct((nz,) + meta.shape, jnp.float32),
        ),
        in_specs=[pl.BlockSpec(memory_space=pltpu.VMEM)] * 2,
        out_specs=[pl.BlockSpec(memory_space=pltpu.VMEM)] * 2,
        scratch_shapes=[
            pltpu.VMEM((nz,) + x.shape, jnp.bfloat16),
            pltpu.VMEM((nz, ep, local_experts, SLOTS, width), jnp.bfloat16),
            dma((nz,)), dma((nz,)), dma((nz,)), dma((nz,)),
            dma((nz, ep)), dma((nz, ep)), dma((nz, ep)), dma((nz, ep)),
        ],
        compiler_params=pltpu.CompilerParams(
            collective_id=0, has_side_effects=True, vmem_limit_bytes=60 * 1024 * 1024
        ),
        cost_estimate=pl.CostEstimate(
            flops=30_000_000_000, bytes_accessed=20_000_000, transcendentals=0
        ),
    )(x, meta)


def combine_kernel(
    ep, nz, local_experts, part_ref, metas_ref, out_ref, pair, sums, rows_in, outbox, final,
    ps, pr, cs, cr, fs, fr,
):
    e, t = lax.axis_index("ep"), lax.axis_index("tp")
    z, c = t // CORES, t % CORES
    partner = (e, z * CORES + 1 - c)
    tokens = out_ref.shape[0]
    width = out_ref.shape[1]
    greet(e, t, ep, nz)
    group = local_experts * SLOTS

    def column(j):
        return lax.rem(e + j, ep)

    def target(k):
        return lax.rem(z - k + nz, nz)

    def pair_copy(k, j):
        return pltpu.make_async_remote_copy(
            src_ref=part_ref.at[:, 1 - c, column(j), target(k)], dst_ref=pair.at[k, j],
            send_sem=ps.at[k, j], recv_sem=pr.at[k, j], device_id=partner, device_id_type=MESH,
        )

    def row_copy(k, j):
        return pltpu.make_async_remote_copy(
            src_ref=sums.at[k, j], dst_ref=rows_in.at[k, j],
            send_sem=cs.at[k, j], recv_sem=cr.at[k, j],
            device_id=(column(j), t), device_id_type=MESH,
        )

    def final_copy(k):
        return pltpu.make_async_remote_copy(
            src_ref=outbox.at[k], dst_ref=final.at[k], send_sem=fs.at[k], recv_sem=fr.at[k],
            device_id=(e, target(k) * CORES + c), device_id_type=MESH,
        )

    far_first = [2] + [j for j in range(1, ep) if j != 2] if ep > 2 else list(range(1, ep))
    order = sorted(range(1, nz), key=lambda k: -min(k, nz - k)) + [0]
    for k in order:
        for j in far_first + [0]:
            pair_copy(k, j).start()

    def add_pairs(k):
        for j in far_first + [0]:
            pair_copy(k, j).wait_recv()
            sums[k, j] = (
                part_ref[:, c, column(j), target(k)].astype(jnp.float32)
                + pair[k, j].astype(jnp.float32)
            ).astype(jnp.bfloat16)
            if j > 0:
                row_copy(k, j).start()

    def combine(k):
        info = metas_ref[k]
        total = jnp.zeros((tokens, width), jnp.float32)
        for j in range(ep):
            if j > 0:
                row_copy(k, j).wait_recv()
            held = (sums if j == 0 else rows_in)[k, j].reshape(group, width)
            first = (lax.rem(e - j + ep, ep) * group).astype(jnp.float32)
            slot = first + lax.broadcasted_iota(jnp.int32, (group, tokens), 0).astype(jnp.float32)
            weight = jnp.where(slot == info[0:1, :tokens], info[2:3, :tokens], 0.0) + jnp.where(
                slot == info[1:2, :tokens], info[3:4, :tokens], 0.0
            )
            high = weight.astype(jnp.bfloat16)
            low = (weight - high.astype(jnp.float32)).astype(jnp.bfloat16)
            for piece in (high, low):
                total = total + lax.dot_general(
                    piece, held, (((0,), (0,)), ((), ())), preferred_element_type=jnp.float32
                )
        return total

    for k in order:
        add_pairs(k)
    for k in order[:-1]:
        outbox[k] = combine(k).astype(jnp.bfloat16)
        final_copy(k).start()
    total = combine(0)
    for k in order[:-1]:
        final_copy(k).wait_recv()
        total = total + final[k].astype(jnp.float32)
    out_ref[...] = total.astype(jnp.bfloat16)
    for k in range(nz):
        if k > 0:
            final_copy(k).wait_send()
        for j in range(ep):
            pair_copy(k, j).wait_send()
            if j > 0:
                row_copy(k, j).wait_send()


def combine_rows(part, metas, tokens, ep, nz, local_experts):
    width = part.shape[-1]
    dma = pltpu.SemaphoreType.DMA
    box = (nz, ep, local_experts, SLOTS, width)
    return pl.pallas_call(
        functools.partial(combine_kernel, ep, nz, local_experts),
        out_shape=jax.ShapeDtypeStruct((tokens, width), jnp.bfloat16),
        in_specs=[pl.BlockSpec(memory_space=pltpu.VMEM)] * 2,
        out_specs=pl.BlockSpec(memory_space=pltpu.VMEM),
        scratch_shapes=[
            pltpu.VMEM(box, jnp.bfloat16),
            pltpu.VMEM(box, jnp.bfloat16),
            pltpu.VMEM(box, jnp.bfloat16),
            pltpu.VMEM((nz, tokens, width), jnp.bfloat16),
            pltpu.VMEM((nz, tokens, width), jnp.bfloat16),
            dma((nz, ep)), dma((nz, ep)), dma((nz, ep)), dma((nz, ep)), dma((nz,)), dma((nz,)),
        ],
        compiler_params=pltpu.CompilerParams(
            collective_id=1, has_side_effects=True, vmem_limit_bytes=60 * 1024 * 1024
        ),
        cost_estimate=pl.CostEstimate(
            flops=40_000_000_000, bytes_accessed=20_000_000, transcendentals=0
        ),
    )(part, metas)


def local(
    queries, key_vectors, value_vectors, cumulative_gate, out_weight, expert_tokens, norm_gain,
    gate_weight, up_weight, down_weight, expert_choice, route_weights,
):
    ep, nz = lax.axis_size("ep"), lax.axis_size("tp") // CORES
    tokens, width = expert_tokens.shape
    local_experts = gate_weight.shape[0]
    gate_high = lax.reduce_precision(cumulative_gate, 8, 7)
    gate_rest = cumulative_gate - gate_high
    gate_mid = lax.reduce_precision(gate_rest, 8, 7)
    gate_low = gate_rest - gate_mid
    shared = jnp.concatenate(
        [key_vectors, value_vectors]
        + [piece.astype(jnp.bfloat16) for piece in (gate_high, gate_mid, gate_low)],
        axis=1,
    )
    all_rows = lax.all_gather(shared, "ep", axis=0, tiled=True)

    tokens_float = expert_tokens.astype(jnp.float32)
    normed = (
        tokens_float
        * lax.rsqrt(jnp.mean(tokens_float * tokens_float, axis=1, keepdims=True) + eps_norm)
        * norm_gain
    ).astype(jnp.bfloat16)
    flat_ids = expert_choice.reshape(-1)
    one_hot = (flat_ids[:, None] == jnp.arange(ep * local_experts, dtype=jnp.int32)[None, :]).astype(
        jnp.float32
    )
    position = jnp.arange(flat_ids.shape[0], dtype=jnp.int32)
    earlier = (position[:, None] > position[None, :]).astype(jnp.float32)
    slot_rank = jnp.sum(jnp.dot(earlier, one_hot) * one_hot, axis=1)
    slot_ids = (flat_ids.astype(jnp.float32) * SLOTS + slot_rank).reshape(tokens, -1)
    meta = jnp.concatenate([slot_ids.T, route_weights.T], axis=0)
    meta = jnp.pad(meta, ((0, 8 - meta.shape[0]), (0, -tokens % 128)), constant_values=-1.0)
    grouped, metas = dispatch(normed, meta, ep, nz, local_experts)

    kept = queries.shape[1]
    heads_here = cumulative_gate.shape[1]
    grouped, all_rows = lax.optimization_barrier((grouped, all_rows))
    key_rows, value_rows = all_rows[:, :kept], all_rows[:, kept : 2 * kept]
    pieces = all_rows[:, 2 * kept :].astype(jnp.float32)
    gate_rows = (
        pieces[:, :heads_here] + pieces[:, heads_here : 2 * heads_here]
    ) + pieces[:, 2 * heads_here :]
    block_rows = queries.shape[0]
    first_query = lax.axis_index("ep") * block_rows
    query_pos = first_query + jnp.arange(block_rows, dtype=jnp.int32)
    last_query = first_query + block_rows - 1
    carried = (
        jnp.full((heads_here, block_rows), floor_score, jnp.float32),
        jnp.zeros((heads_here, block_rows), jnp.float32),
        jnp.zeros((block_rows, kept), jnp.float32),
    )

    def one_shard(inner_state, shard_index):
        offset = shard_index * block_rows
        shard_keys = lax.dynamic_slice_in_dim(key_rows, offset, block_rows, 0)
        shard_values = lax.dynamic_slice_in_dim(value_rows, offset, block_rows, 0)
        shard_gates = lax.dynamic_slice_in_dim(gate_rows, offset, block_rows, 0)
        updated = lax.cond(
            offset <= last_query,
            lambda held_state: attend_shard(
                held_state, queries, cumulative_gate, query_pos, shard_keys, shard_values,
                shard_gates, offset,
            ),
            lambda held_state: held_state,
            inner_state,
        )
        return (updated, None)

    carried, unused = lax.scan(one_shard, carried, jnp.arange(ep, dtype=jnp.int32))
    final_peak, final_sum, final_accum = carried
    attention = (
        (final_accum.reshape(block_rows, heads_here, -1) / final_sum.T[:, :, None])
        .reshape(block_rows, -1)
        .astype(jnp.bfloat16)
    )
    mixed = head_term(attention, out_weight).astype(jnp.bfloat16)
    grouped, mixed = lax.optimization_barrier((grouped, mixed))
    mixer_output = lax.psum_scatter(mixed, "tp", scatter_dimension=0, tiled=True)

    rows_in = grouped.reshape(local_experts, -1, width)
    gate_pre = jnp.minimum(
        jnp.einsum("ecd,edf->ecf", rows_in, gate_weight, preferred_element_type=jnp.float32),
        clamp_limit,
    )
    up_pre = jnp.clip(
        jnp.einsum("ecd,edf->ecf", rows_in, up_weight, preferred_element_type=jnp.float32),
        -clamp_limit,
        clamp_limit,
    )
    activation = (gate_pre * jax.nn.sigmoid(sig_alpha * gate_pre) * (up_pre + 1.0)).astype(
        jnp.bfloat16
    )
    part = jnp.einsum(
        "eci,eid->ecd", activation, down_weight, preferred_element_type=jnp.float32
    ).astype(jnp.bfloat16)
    expert_output = combine_rows(part.reshape(grouped.shape), metas, tokens, ep, nz, local_experts)
    return (mixer_output, expert_output)


def solution(mesh):
    placed = (
        P("ep", "tp"),
        P("ep", "tp"),
        P("ep", "tp"),
        P("ep", "tp"),
        P("tp", None),
        P(("ep", "tp"), None),
        P(),
        P("ep", None, "tp"),
        P("ep", None, "tp"),
        P("ep", "tp", None),
        P(("ep", "tp"), None),
        P(("ep", "tp"), None),
    )
    return jax.shard_map(
        local,
        mesh=mesh,
        in_specs=placed,
        out_specs=(P(("ep", "tp"), None), P(("ep", "tp"), None)),
        check_vma=False,
    )
```

```python
import functools
import math

import jax
import jax.numpy as jnp
from jax import lax
from jax.experimental import pallas as pl
from jax.experimental.pallas import tpu as pltpu
from jax.sharding import PartitionSpec as P

SLOTS = 16
CORES = 2
MESH = pl.DeviceIdType.MESH


eps_norm = 1e-05
clamp_limit = 7.0
sig_alpha = 1.702
floor_score = -1e30


def attend_shard(
    carried, queries, query_gates, query_pos, key_rows, value_rows, key_gates, key_start
):
    running_max, running_sum, accum = carried
    heads_here = query_gates.shape[1]
    head_width = queries.shape[1] // heads_here
    score_scale = 1.0 / math.sqrt(head_width)
    key_pos = key_start + jnp.arange(key_rows.shape[0], dtype=jnp.int32)
    causal = key_pos[None, :] <= query_pos[:, None]
    maxima = []
    totals = []
    blocks = []
    for head_index in range(heads_here):
        first_column = head_index * head_width
        last_column = first_column + head_width
        scores = (
            jnp.einsum(
                "qd,kd->qk",
                queries[:, first_column:last_column],
                key_rows[:, first_column:last_column],
                preferred_element_type=jnp.float32,
            )
            * score_scale
        )
        scores = (
            scores + query_gates[:, head_index : head_index + 1] - key_gates[:, head_index][None, :]
        )
        scores = jnp.where(causal, scores, floor_score)
        new_peak = jnp.maximum(running_max[head_index], jnp.max(scores, axis=1))
        weights = jnp.where(causal, jnp.exp(scores - new_peak[:, None]), 0.0)
        shrink = jnp.exp(running_max[head_index] - new_peak)
        maxima.append(new_peak)
        totals.append(running_sum[head_index] * shrink + jnp.sum(weights, axis=1))
        blocks.append(
            accum[:, first_column:last_column] * shrink[:, None]
            + jnp.dot(
                weights.astype(jnp.bfloat16),
                value_rows[:, first_column:last_column],
                preferred_element_type=jnp.float32,
            )
        )
    return (jnp.stack(maxima), jnp.stack(totals), jnp.concatenate(blocks, axis=1))


def head_term(attention, out_weight):
    return jnp.dot(attention, out_weight, preferred_element_type=jnp.float32)


def greet(e, t, ep, nz):
    z, c = t // CORES, t % CORES
    barrier = pltpu.get_barrier_semaphore()
    peers = [(e, z * CORES + 1 - c)]
    peers += [(e, lax.rem(z + k, nz) * CORES + c) for k in range(1, nz)]
    peers += [(lax.rem(e + j, ep), t) for j in range(1, ep)]
    for peer in peers:
        pl.semaphore_signal(barrier, inc=1, device_id=peer, device_id_type=MESH)
    pl.semaphore_wait(barrier, len(peers))


def expert_kernel(
    ep, nz, local_experts, x_ref, meta_ref, gate_ref, up_ref, down_ref, out_ref,
    metas, xbuf, outbox, rows, pair, rows_in, finalbox, final, gate_w, up_w, down_w,
    xs, xr, ms, mr, cs, cr, ds, dr, ps, pr, bs, br, fs, fr, ws,
):
    e, t = lax.axis_index("ep"), lax.axis_index("tp")
    z, c = t // CORES, t % CORES
    partner = (e, z * CORES + 1 - c)
    tokens, width = x_ref.shape
    group = local_experts * SLOTS
    greet(e, t, ep, nz)

    def column(j):
        return lax.rem(e + j, ep)

    def behind(j):
        return lax.rem(e - j + ep, ep)

    def remote(src, dst, send, recv, device):
        return pltpu.make_async_remote_copy(
            src_ref=src, dst_ref=dst, send_sem=send, recv_sem=recv,
            device_id=device, device_id_type=MESH,
        )

    def token_copy(k):
        dest = (e, lax.rem(z + k, nz) * CORES + c)
        return (
            remote(meta_ref, metas.at[k], ms.at[k], mr.at[k], dest),
            remote(x_ref, xbuf.at[k], xs.at[k], xr.at[k], dest),
        )

    def row_copy(k, j):
        return remote(
            outbox.at[k, column(j)], rows.at[k, :, c, e], cs.at[k, j], cr.at[k, j], (column(j), t)
        )

    def share_copy(k, j):
        block = rows.at[k, :, c, behind(j)]
        return remote(block, block, ds.at[k, j], dr.at[k, j], partner)

    def share_arrival(k, j):
        block = rows.at[k, :, 1 - c, behind(j)]
        return remote(block, block, ds.at[k, j], dr.at[k, j], partner)

    def pair_copy(k, j):
        return remote(
            rows.at[k, :, 1 - c, column(j)], pair.at[k, j], ps.at[k, j], pr.at[k, j], partner
        )

    def back_copy(k, j):
        return remote(
            rows.at[k, :, c, column(j)], rows_in.at[k, j], bs.at[k, j], br.at[k, j], (column(j), t)
        )

    def final_copy(k):
        dest = (e, lax.rem(z - k + nz, nz) * CORES + c)
        return remote(finalbox.at[k], final.at[k], fs.at[k], fr.at[k], dest)

    order = [0] + sorted(range(1, nz), key=lambda k: -min(k, nz - k))
    columns = [2] + [j for j in range(1, ep) if j != 2] if ep > 2 else list(range(1, ep))
    for k in order[1:]:
        for copy in token_copy(k):
            copy.start()
    loads = [
        pltpu.make_async_copy(source, held, ws.at[n])
        for n, (source, held) in enumerate(
            ((gate_ref, gate_w), (up_ref, up_w), (down_ref, down_w))
        )
    ]
    for load in loads:
        load.start()
    metas[0] = meta_ref[...]

    def select(k):
        if k > 0:
            for copy in token_copy(k):
                copy.wait_recv()
        block = x_ref if k == 0 else xbuf.at[k]
        info = metas[k]
        slot = lax.broadcasted_iota(jnp.int32, (ep * group, tokens), 0).astype(jnp.float32)
        chosen = (slot == info[0:1, :tokens]) | (slot == info[1:2, :tokens])
        picked = jnp.dot(
            jnp.where(chosen, 1.0, 0.0).astype(jnp.bfloat16), block[...],
            preferred_element_type=jnp.float32,
        ).astype(jnp.bfloat16)
        outbox[k] = picked.reshape(ep, local_experts, SLOTS, width)
        for j in columns:
            row_copy(k, j).start()
        rows[k, :, c, e] = outbox[k, e]
        share_copy(k, 0).start()

    def pass_on(k):
        for j in columns:
            row_copy(k, j).wait_recv()
            share_copy(k, j).start()

    def compute(k):
        for j in range(ep):
            share_arrival(k, j).wait_recv()
            share_copy(k, j).wait_send()

        def one_expert(n, carry):
            held = rows[k, n].reshape(CORES * ep * SLOTS, width)
            gate_pre = jnp.minimum(
                jnp.dot(held, gate_w[n], preferred_element_type=jnp.float32), clamp_limit
            )
            up_pre = jnp.clip(
                jnp.dot(held, up_w[n], preferred_element_type=jnp.float32),
                -clamp_limit,
                clamp_limit,
            )
            active = (gate_pre * jax.nn.sigmoid(sig_alpha * gate_pre) * (up_pre + 1.0)).astype(
                jnp.bfloat16
            )
            part = jnp.dot(active, down_w[n], preferred_element_type=jnp.float32)
            rows[k, n] = part.astype(jnp.bfloat16).reshape(CORES, ep, SLOTS, width)
            return carry

        lax.fori_loop(0, local_experts, one_expert, 0)
        for j in columns + [0]:
            pair_copy(k, j).start()

    def add_pairs(k):
        for j in columns + [0]:
            pair_copy(k, j).wait_recv()
            total = (
                rows[k, :, c, column(j)].astype(jnp.float32) + pair[k, j].astype(jnp.float32)
            ).astype(jnp.bfloat16)
            if j > 0:
                rows[k, :, c, column(j)] = total
                back_copy(k, j).start()
            else:
                rows_in[k, 0] = total

    def combine(k):
        for j in columns:
            back_copy(k, j).wait_recv()
        info = metas[k]
        slot = jnp.concatenate(
            [
                (behind(j) * group + lax.broadcasted_iota(jnp.int32, (group, tokens), 0)).astype(
                    jnp.float32
                )
                for j in range(ep)
            ],
            axis=0,
        )
        weight = jnp.where(slot == info[0:1, :tokens], info[2:3, :tokens], 0.0) + jnp.where(
            slot == info[1:2, :tokens], info[3:4, :tokens], 0.0
        )
        high = weight.astype(jnp.bfloat16)
        low = (weight - high.astype(jnp.float32)).astype(jnp.bfloat16)
        held = rows_in[k].reshape(ep * group, width)
        total = jnp.zeros((tokens, width), jnp.float32)
        for piece in (high, low):
            total = total + lax.dot_general(
                piece, held, (((0,), (0,)), ((), ())), preferred_element_type=jnp.float32
            )
        return total

    for k in order:
        select(k)
    for load in loads:
        load.wait()
    for n, k in enumerate(order):
        pass_on(k)
        if n > 0:
            add_pairs(order[n - 1])
        compute(k)
    add_pairs(order[-1])
    total = combine(0)
    for k in order[1:]:
        finalbox[k] = combine(k).astype(jnp.bfloat16)
        final_copy(k).start()
    for k in order[1:]:
        final_copy(k).wait_recv()
        total = total + final[k].astype(jnp.float32)
    out_ref[...] = total.astype(jnp.bfloat16)
    for k in range(nz):
        if k > 0:
            final_copy(k).wait_send()
            for copy in token_copy(k):
                copy.wait_send()
        for j in range(ep):
            pair_copy(k, j).wait_send()
            if j > 0:
                row_copy(k, j).wait_send()
                back_copy(k, j).wait_send()


def run_experts(x, meta, gate_weight, up_weight, down_weight, ep, nz):
    local_experts = gate_weight.shape[0]
    width = x.shape[1]
    dma = pltpu.SemaphoreType.DMA
    box = (nz, ep, local_experts, SLOTS, width)
    vmem = pl.BlockSpec(memory_space=pltpu.VMEM)
    held = pl.BlockSpec(memory_space=pl.ANY)
    return pl.pallas_call(
        functools.partial(expert_kernel, ep, nz, local_experts),
        out_shape=jax.ShapeDtypeStruct(x.shape, jnp.bfloat16),
        in_specs=[vmem, vmem, held, held, held],
        out_specs=vmem,
        scratch_shapes=[
            pltpu.VMEM((nz,) + meta.shape, jnp.float32),
            pltpu.VMEM((nz,) + x.shape, jnp.bfloat16),
            pltpu.VMEM(box, jnp.bfloat16),
            pltpu.VMEM((nz, local_experts, CORES, ep, SLOTS, width), jnp.bfloat16),
            pltpu.VMEM(box, jnp.bfloat16),
            pltpu.VMEM(box, jnp.bfloat16),
            pltpu.VMEM((nz,) + x.shape, jnp.bfloat16),
            pltpu.VMEM((nz,) + x.shape, jnp.bfloat16),
            pltpu.VMEM(gate_weight.shape, jnp.bfloat16),
            pltpu.VMEM(up_weight.shape, jnp.bfloat16),
            pltpu.VMEM(down_weight.shape, jnp.bfloat16),
            dma((nz,)), dma((nz,)), dma((nz,)), dma((nz,)),
            dma((nz, ep)), dma((nz, ep)), dma((nz, ep)), dma((nz, ep)),
            dma((nz, ep)), dma((nz, ep)), dma((nz, ep)), dma((nz, ep)),
            dma((nz,)), dma((nz,)), dma((3,)),
        ],
        compiler_params=pltpu.CompilerParams(
            collective_id=0, has_side_effects=True, vmem_limit_bytes=63 * 1024 * 1024
        ),
        cost_estimate=pl.CostEstimate(
            flops=60_000_000_000, bytes_accessed=20_000_000, transcendentals=0
        ),
    )(x, meta, gate_weight, up_weight, down_weight)


def local(
    queries, key_vectors, value_vectors, cumulative_gate, out_weight, expert_tokens, norm_gain,
    gate_weight, up_weight, down_weight, expert_choice, route_weights,
):
    ep, nz = lax.axis_size("ep"), lax.axis_size("tp") // CORES
    tokens, width = expert_tokens.shape
    local_experts = gate_weight.shape[0]
    gate_high = lax.reduce_precision(cumulative_gate, 8, 7)
    gate_rest = cumulative_gate - gate_high
    gate_mid = lax.reduce_precision(gate_rest, 8, 7)
    gate_low = gate_rest - gate_mid
    keyed = jnp.concatenate(
        [key_vectors]
        + [piece.astype(jnp.bfloat16) for piece in (gate_high, gate_mid, gate_low)],
        axis=1,
    )
    all_keyed = lax.all_gather(keyed, "ep", axis=0, tiled=True)
    value_rows = lax.all_gather(value_vectors, "ep", axis=0, tiled=True)

    tokens_float = expert_tokens.astype(jnp.float32)
    normed = (
        tokens_float
        * lax.rsqrt(jnp.mean(tokens_float * tokens_float, axis=1, keepdims=True) + eps_norm)
        * norm_gain
    ).astype(jnp.bfloat16)
    flat_ids = expert_choice.reshape(-1)
    one_hot = (flat_ids[:, None] == jnp.arange(ep * local_experts, dtype=jnp.int32)[None, :]).astype(
        jnp.float32
    )
    position = jnp.arange(flat_ids.shape[0], dtype=jnp.int32)
    earlier = (position[:, None] > position[None, :]).astype(jnp.float32)
    slot_rank = jnp.sum(jnp.dot(earlier, one_hot) * one_hot, axis=1)
    slot_ids = (flat_ids.astype(jnp.float32) * SLOTS + slot_rank).reshape(tokens, -1)
    meta = jnp.concatenate([slot_ids.T, route_weights.T], axis=0)
    meta = jnp.pad(meta, ((0, 8 - meta.shape[0]), (0, -tokens % 128)), constant_values=-1.0)

    kept = queries.shape[1]
    heads_here = cumulative_gate.shape[1]
    key_rows = all_keyed[:, :kept]
    pieces = all_keyed[:, kept:].astype(jnp.float32)
    gate_rows = (
        pieces[:, :heads_here] + pieces[:, heads_here : 2 * heads_here]
    ) + pieces[:, 2 * heads_here :]
    block_rows = queries.shape[0]
    first_query = lax.axis_index("ep") * block_rows
    query_pos = first_query + jnp.arange(block_rows, dtype=jnp.int32)
    last_query = first_query + block_rows - 1
    carried = (
        jnp.full((heads_here, block_rows), floor_score, jnp.float32),
        jnp.zeros((heads_here, block_rows), jnp.float32),
        jnp.zeros((block_rows, kept), jnp.float32),
    )

    def one_shard(inner_state, shard_index):
        offset = shard_index * block_rows
        shard_keys = lax.dynamic_slice_in_dim(key_rows, offset, block_rows, 0)
        shard_values = lax.dynamic_slice_in_dim(value_rows, offset, block_rows, 0)
        shard_gates = lax.dynamic_slice_in_dim(gate_rows, offset, block_rows, 0)
        updated = lax.cond(
            offset <= last_query,
            lambda held_state: attend_shard(
                held_state, queries, cumulative_gate, query_pos, shard_keys, shard_values,
                shard_gates, offset,
            ),
            lambda held_state: held_state,
            inner_state,
        )
        return (updated, None)

    carried, unused = lax.scan(one_shard, carried, jnp.arange(ep, dtype=jnp.int32))
    final_peak, final_sum, final_accum = carried
    attention = (
        (final_accum.reshape(block_rows, heads_here, -1) / final_sum.T[:, :, None])
        .reshape(block_rows, -1)
        .astype(jnp.bfloat16)
    )
    mixed = head_term(attention, out_weight).astype(jnp.bfloat16)
    normed, meta, mixed = lax.optimization_barrier((normed, meta, mixed))
    mixer_output = lax.psum_scatter(mixed, "tp", scatter_dimension=0, tiled=True)
    expert_output = run_experts(normed, meta, gate_weight, up_weight, down_weight, ep, nz)
    return (mixer_output, expert_output)


def solution(mesh):
    placed = (
        P("ep", "tp"),
        P("ep", "tp"),
        P("ep", "tp"),
        P("ep", "tp"),
        P("tp", None),
        P(("ep", "tp"), None),
        P(),
        P("ep", None, "tp"),
        P("ep", None, "tp"),
        P("ep", "tp", None),
        P(("ep", "tp"), None),
        P(("ep", "tp"), None),
    )
    return jax.shard_map(
        local,
        mesh=mesh,
        in_specs=placed,
        out_specs=(P(("ep", "tp"), None), P(("ep", "tp"), None)),
        check_vma=False,
    )
```
